32 devices in a mesh: sp: 8 (over z, x), tp: 4 (over y, core).
Axes of the slice: x: 2, y: 2, z: 4, core: 2. Of those that a mesh axis runs over, the one named last changes fastest.
Arguments:
- queries: bfloat16 [1024, 2048], P('sp', 'tp'), may hold values from -440 to 440
- key_rows: bfloat16 [1024, 1024], P('sp', 'tp'), may hold values from -6 to 6
- value_rows: bfloat16 [1024, 1024], P('sp', 'tp'), may hold values from -6 to 6
- sink_logits: float32 [32], P('tp'), may hold values from -6 to 6
- out_weight: bfloat16 [2048, 2048], P('tp'), may hold values from -0.125 to 0.125
- residual: bfloat16 [1024, 2048], P('sp'), may hold values from -3 to 3
- norm_gain: float32 [2048], replicated, may hold values from 0.1 to 1.9
- routes: int32 [1024, 2], P('sp'), may hold values from 0 to 7, all different within a row; in each aligned block of 128 rows (0 to 127, 128 to 255, ...) at most 64 rows name the same one
- route_weights: float32 [1024, 2], P('sp'), may hold values from 0.2 to 1
- gate_weight: bfloat16 [8, 2048, 4096], P('sp', None, 'tp'), may hold values from -0.125 to 0.125
- up_weight: bfloat16 [8, 2048, 4096], P('sp', None, 'tp'), may hold values from -0.125 to 0.125
- down_weight: bfloat16 [8, 4096, 2048], P('sp', 'tp'), may hold values from -0.09375 to 0.09375
Outputs:
- layer_out: bfloat16 [1024, 2048], P('sp')
The draws below stay inside these ranges and needn't reach their ends.
Inputs may be any that keep to these rules, and one draw needn't show every extreme that they name: `routes`: each row names 2 different experts. In each aligned block of 128 rows (the rows of one index of sp) no expert is named by more than 64 rows, a bound that some block reaches.
All inputs are finite; a program needn't handle non-finite values.
Results may differ from the reference program's by a relative error of at most 0.02.
Values may be sent and summed in bfloat16 or wider, within the bound.
No kernel may reach another device: no remote copies, remote signals or barrier semaphores. Data moves between devices by JAX's collectives and lax.ppermute only.
A program may use at most 64 MiB of HBM per device.

```python
import math
import jax
import jax.numpy as jnp
import numpy as np
from jax import lax

D = 2048
HEAD_DIM = 64
QH = 32
KVH = 16
WINDOW = 128
FF = 4096
TOP = 2
TOK_DEV = 128
TOKENS = 1024
EXPERTS = 8
CAP = 64
N_SP = 8
N_TP = 4


def plant_keys(key):
    key_draw = jax.random.normal(jax.random.fold_in(key, 7), (TOKENS, KVH * HEAD_DIM), jnp.float32)
    return jnp.clip(key_draw, -6.0, 6.0)


def draw_key_rows(key, part):
    key_draw = plant_keys(key)
    return key_draw.astype(jnp.bfloat16)


def draw_queries(key, part):
    base = jax.random.normal(jax.random.fold_in(key, 8), (TOKENS, QH * HEAD_DIM), jnp.float32)
    base = jnp.clip(base, -6.0, 6.0)
    return base.astype(jnp.bfloat16)


def levels(key, extent, cuts, smallest, top_value):
    level = 1.0
    for axis_at, shards_of in cuts:
        steps = jax.random.uniform(jax.random.fold_in(jax.random.fold_in(key, 6), axis_at), (shards_of,), jnp.float32, smallest / len(cuts), top_value / len(cuts))
        level = level * jnp.repeat(jnp.exp(steps), extent[axis_at] // shards_of).reshape((-1,) + (1,) * (len(extent) - 1 - axis_at))
    return level


def deal_out(rng, own, number, rows, amount, top, limit, skew):
    ranking = jax.random.permutation(rng, amount)
    heavy_load, common = portions_of(amount, rows * top, limit, skew, True), portions_of(amount, rows * top, limit, skew, False)
    places = jnp.arange(amount)

    def named(tallies, turn):
        used = int((tallies > 0).sum())
        fixed = max(1, used // 4)
        moved = fixed + (places - fixed + turn * (used - fixed)) % max(1, amount - fixed)
        return jnp.zeros((amount,), jnp.int32).at[ranking[jnp.where(places < fixed, places, moved)]].set(jnp.asarray(tallies, jnp.int32))

    tallies = jnp.where(number % 4 == 0, named(heavy_load, number // 4), named(common, number - number // 4 - 1))
    mixed = jax.random.permutation(jax.random.fold_in(own, 3), amount)
    source_of, taker = mixed[0:amount // 2 * 2:2], mixed[1:amount // 2 * 2:2]
    margin = jnp.minimum(tallies[source_of] - 1, limit - tallies[taker]) // 2
    margin = jnp.where((source_of == ranking[0]) | (taker == ranking[0]) | (tallies[taker] == 0), 0, jnp.maximum(margin, 0))
    moved = jax.random.randint(jax.random.fold_in(own, 4), (amount // 2,), 0, 1 << 20) % (margin + 1)
    tallies = tallies.at[source_of].add(-moved).at[taker].add(moved)
    items = jnp.searchsorted(jnp.cumsum(tallies), jnp.arange(rows * top), side="right").astype(jnp.int32)
    grid = items.reshape(top, rows).T
    grid = grid[jax.random.permutation(jax.random.fold_in(own, 1), rows)]
    turn = jax.random.randint(jax.random.fold_in(own, 2), (rows, 1), 0, top)
    return jnp.take_along_axis(grid, (jnp.arange(top)[None, :] + turn) % top, axis=1)


def portions_of(amount, total, limit, slope, full):
    weights = [(1 << 20) // math.isqrt(standing ** slope) + 1 for standing in range(1, amount + 1)]
    largest = limit if full else min(limit, max(-(-total // amount), total * weights[0] // sum(weights)))
    least = 1 if total - largest >= amount - 1 else 0
    counts, surplus = [largest] + [least] * (amount - 1), total - largest - least * (amount - 1)
    while surplus > 0:
        movable = [i for i in range(1, amount) if counts[i] < largest] or [i for i in range(1, amount) if counts[i] < limit]
        whole, left = sum([weights[i] for i in movable]), surplus
        for i in movable:
            addition = min(limit - counts[i], max(1, left * weights[i] // whole), surplus)
            counts[i] = counts[i] + addition
            surplus = surplus - addition
    return np.array(counts)


def noise(rng, extent, deviation, limit, shards=(), kind=jnp.bfloat16):
    level = levels(rng, extent, shards, -0.22, 0.18) if shards else 1.0
    result = jax.random.normal(rng, extent, jnp.float32) * deviation * level
    return jnp.minimum(jnp.maximum(result, -limit), limit).astype(kind)


def setup_inputs(seed: int = 0) -> dict:
    key_of = jax.random.split(jax.random.key(seed), 13)
    queries = draw_queries(jax.random.fold_in(key_of[12], 71), 0)
    key_rows = draw_key_rows(jax.random.fold_in(key_of[12], 71), 0)
    value_rows = noise(key_of[2], (TOKENS, KVH * HEAD_DIM), 1.0, 6.0, ((0, 8), (1, 4)))
    sink_logits = noise(key_of[3], (QH,), 2.0, 6.0, ((0, 4),), jnp.float32)
    out_weight = noise(key_of[4], (QH * HEAD_DIM, D), (QH * HEAD_DIM) ** -0.5, 0.125, ((0, 4),))
    residual = noise(key_of[5], (TOKENS, D), 0.5, 3.0, ((0, 8),))
    norm_gain = jnp.clip(1.0 + 0.18 * jax.random.normal(key_of[6], (D,), jnp.float32), 0.1, 1.9)
    routes_keys = jax.random.split(jax.random.fold_in(key_of[7], 1), TOKENS // TOK_DEV)
    routes_turns = jax.random.permutation(jax.random.fold_in(key_of[7], 3), TOKENS // TOK_DEV)
    routes = jax.vmap(lambda own, number: deal_out(jax.random.fold_in(key_of[7], 2), own, number, TOK_DEV, EXPERTS, TOP, CAP, 1))(routes_keys, routes_turns).reshape((TOKENS, TOP))
    route_weights = jnp.clip(0.2 + 0.8 * jax.random.uniform(key_of[8], (TOKENS, TOP), jnp.float32) ** levels(key_of[8], (TOKENS, TOP), ((0, 8),), -0.2, 0.2), 0.2, 1.0)
    gate_weight = noise(key_of[9], (EXPERTS, D, FF), D ** -0.5, 0.125, ((0, 8), (2, 4)))
    up_weight = noise(key_of[10], (EXPERTS, D, FF), D ** -0.5, 0.125, ((0, 8), (2, 4)))
    down_weight = noise(key_of[11], (EXPERTS, FF, D), FF ** -0.5, 0.09375, ((0, 8), (1, 4)))
    return dict(queries=queries, key_rows=key_rows, value_rows=value_rows, sink_logits=sink_logits, out_weight=out_weight, residual=residual, norm_gain=norm_gain, routes=routes, route_weights=route_weights, gate_weight=gate_weight, up_weight=up_weight, down_weight=down_weight)


def reference(queries, key_rows, value_rows, sink_logits, out_weight, residual, norm_gain, routes, route_weights, gate_weight, up_weight, down_weight):
    blocks = TOKENS // WINDOW
    group_size = QH // KVH
    zeros_rim = jnp.zeros((WINDOW, KVH * HEAD_DIM), jnp.bfloat16)
    key_ext = jnp.concatenate([zeros_rim, key_rows], axis=0).reshape(blocks + 1, WINDOW, KVH, HEAD_DIM)
    val_ext = jnp.concatenate([zeros_rim, value_rows], axis=0).reshape(blocks + 1, WINDOW, KVH, HEAD_DIM)
    key_pair = jnp.concatenate([key_ext[:-1], key_ext[1:]], axis=1)
    val_pair = jnp.concatenate([val_ext[:-1], val_ext[1:]], axis=1)
    query_blocks = queries.reshape(blocks, WINDOW, KVH, group_size, HEAD_DIM)
    distance = jnp.arange(WINDOW)[:, None] + WINDOW - jnp.arange(2 * WINDOW)[None, :]
    key_global = jnp.arange(blocks)[:, None, None] * WINDOW + jnp.arange(2 * WINDOW)[None, None, :] - WINDOW
    allowed = (distance >= 0)[None] & (distance <= WINDOW)[None] & (key_global >= 0)
    head_ids = jnp.arange(QH)
    slopes = jnp.exp2(-8.0 * (head_ids + 1).astype(jnp.float32) / QH).reshape(KVH, group_size)

    def attend_head(inputs):
        q_head, k_head, v_head, sink_head, slope_head = inputs
        scores = jnp.einsum('bqgd,bcd->bgqc', q_head.astype(jnp.float32), k_head.astype(jnp.float32)) * HEAD_DIM ** (-0.5)
        scores = scores - slope_head[None, :, None, None] * distance.astype(jnp.float32)
        scores = jnp.where(allowed[:, None], scores, -jnp.inf)
        row_peak = lax.optimization_barrier(jnp.max(scores, axis=-1, keepdims=True))
        log_total = row_peak + jnp.log(lax.optimization_barrier(jnp.sum(jnp.exp(scores - row_peak), axis=-1, keepdims=True)))
        probs = jnp.exp(scores - log_total).astype(jnp.bfloat16)
        mixed = jnp.einsum('bgqc,bcd->bqgd', probs.astype(jnp.float32), v_head.astype(jnp.float32))
        keep_factor = jax.nn.sigmoid(log_total[..., 0] - sink_head[None, :, None])
        keep_factor = jnp.transpose(keep_factor, (0, 2, 1))[..., None]
        return (mixed * keep_factor).astype(jnp.bfloat16)
    per_head = lax.map(attend_head, (jnp.moveaxis(query_blocks, 2, 0), jnp.moveaxis(key_pair, 2, 0), jnp.moveaxis(val_pair, 2, 0), sink_logits.reshape(KVH, group_size), slopes))
    attended = jnp.moveaxis(per_head, 0, 2).reshape(TOKENS, QH * HEAD_DIM)
    columns = QH * HEAD_DIM // N_TP
    head_total = jnp.zeros((TOKENS, D), jnp.float32)
    for piece_id in range(N_TP):
        partial_value = jnp.dot(attended[:, piece_id * columns:(piece_id + 1) * columns], out_weight[piece_id * columns:(piece_id + 1) * columns], preferred_element_type=jnp.float32)
        head_total = head_total + lax.optimization_barrier(partial_value.astype(jnp.bfloat16)).astype(jnp.float32)
    mixed_state = (residual.astype(jnp.float32) + head_total).astype(jnp.bfloat16)
    state32 = mixed_state.astype(jnp.float32)
    normed = (state32 * lax.rsqrt(lax.optimization_barrier(jnp.mean(state32 * state32, axis=-1, keepdims=True)) + 1e-06) * norm_gain).astype(jnp.bfloat16)
    slots = N_SP * CAP
    flat_routes = routes.reshape(-1).astype(jnp.int32)
    token_of = (jnp.arange(TOKENS * TOP) // TOP).astype(jnp.int32)
    member = (flat_routes[:, None] == jnp.arange(EXPERTS)[None, :]).astype(jnp.int32)
    slot_rank = lax.optimization_barrier(jnp.sum((jnp.cumsum(member, axis=0) - 1) * member, axis=1)).astype(jnp.int32)

    def one_expert(inputs):
        expert_id, w_gate, w_up, w_down = inputs
        target = jnp.where(flat_routes == expert_id, slot_rank, slots).astype(jnp.int32)
        slot_token = jnp.zeros((slots,), jnp.int32).at[target].set(token_of, mode='drop')
        slot_rows = normed[slot_token]
        gate_pre = jnp.dot(slot_rows, w_gate, preferred_element_type=jnp.float32)
        up_pre = jnp.dot(slot_rows, w_up, preferred_element_type=jnp.float32)
        activated = (jax.nn.silu(gate_pre) * up_pre).astype(jnp.bfloat16)
        act_groups = activated.reshape(slots, N_TP, FF // N_TP).astype(jnp.float32)
        down_groups = w_down.reshape(N_TP, FF // N_TP, D).astype(jnp.float32)
        parts = jnp.einsum('mpf,pfd->pmd', act_groups, down_groups)
        parts = lax.optimization_barrier(parts.astype(jnp.bfloat16)).astype(jnp.float32)
        return lax.optimization_barrier(jnp.sum(parts, axis=0)).astype(jnp.bfloat16)
    outputs = lax.map(one_expert, (jnp.arange(EXPERTS, dtype=jnp.int32), gate_weight, up_weight, down_weight))
    flat_index = (flat_routes * slots + slot_rank).astype(jnp.int32)
    picked = outputs.reshape(EXPERTS * slots, D)[flat_index].reshape(TOKENS, TOP, D)
    expert_mix = lax.optimization_barrier(jnp.sum(route_weights[..., None] * picked.astype(jnp.float32), axis=1))
    return (state32 + expert_mix).astype(jnp.bfloat16)
```

```python
import functools

import jax
import jax.numpy as jnp
from jax import lax
from jax.experimental import pallas as pl
from jax.experimental.pallas import tpu as pltpu
from jax.sharding import PartitionSpec as P

HEAD_DIM = 64
QH = 32
WINDOW = 128
TOP = 2
CHUNKS = 2
BF = jnp.bfloat16
F32 = jnp.float32
VM = pl.BlockSpec(memory_space=pltpu.VMEM)


def kernel_call(body, outs, scratch=()):
    return pl.pallas_call(
        body,
        out_shape=outs,
        out_specs=jax.tree.map(lambda _: VM, outs),
        scratch_shapes=list(scratch),
    )


def struct(*shape, dtype=BF):
    return jax.ShapeDtypeStruct(shape, dtype)


def place():
    tp = lax.axis_index("tp")
    return lax.axis_index("sp"), tp // 2, tp % 2


def route_body(half, cap, routes, weights, pick, comb):
    at, _, core = place()
    rows = routes.shape[1]
    first, second = routes[0:1, :], routes[1:2, :]
    w_first, w_second = weights[0:1, :], weights[1:2, :]
    earlier = lax.broadcasted_iota(jnp.int32, (rows, rows), 0) < lax.broadcasted_iota(
        jnp.int32, (rows, rows), 1
    )
    earlier = jnp.where(earlier, 1.0, 0.0).astype(BF)
    rank = lax.broadcasted_iota(jnp.int32, (cap, rows), 0)
    for own in range(2):
        side = core if own == 0 else 1 - core
        step = lax.broadcasted_iota(jnp.int32, (half, rows), 0)
        expert = at ^ (2 * (half - 1 - step) + side)
        is_first, is_second = first == expert, second == expert
        named = is_first | is_second
        weight = jnp.where(is_first, w_first, 0.0) + jnp.where(is_second, w_second, 0.0)
        ahead = jnp.dot(
            jnp.where(named, 1.0, 0.0).astype(BF), earlier, preferred_element_type=F32
        ).astype(jnp.int32)
        ahead = jnp.where(named, ahead, -1)
        for k in range(half):
            hit = rank == ahead[k : k + 1, :]
            lo = k * cap
            if own == 0:
                pick[lo : lo + cap, :] = jnp.where(hit, 1.0, 0.0).astype(BF)
            value = jnp.where(hit, weight[k : k + 1, :], 0.0)
            high = value.astype(BF)
            comb[own, 0, lo : lo + cap, :] = high
            comb[own, 1, lo : lo + cap, :] = (value - high.astype(F32)).astype(BF)


def attend_body(tps, q, keys, values, before, sinks, weight, keep, give, attended):
    at, y, core = place()
    rows, kv_width = keys.shape
    heads, kv_heads = q.shape[1] // HEAD_DIM, kv_width // HEAD_DIM
    group = heads // kv_heads
    quarter = weight.shape[1] // tps
    lane = lax.broadcasted_iota(jnp.int32, (1, 128), 1)
    head_id = (lax.axis_index("tp") * heads + lane + 1).astype(F32)
    slopes = jnp.exp2(head_id * (-8.0 / QH))
    row = lax.broadcasted_iota(jnp.int32, (rows, 2 * rows), 0)
    col = lax.broadcasted_iota(jnp.int32, (rows, 2 * rows), 1)
    distance = row + rows - col
    allowed = (distance >= 0) & (distance <= WINDOW) & ((col >= rows) | (at > 0))
    far = distance.astype(F32)
    for g in range(kv_heads):
        here = slice(g * HEAD_DIM, (g + 1) * HEAD_DIM)
        there = slice(kv_width + g * HEAD_DIM, kv_width + (g + 1) * HEAD_DIM)
        k_all = jnp.concatenate([before[:, here], keys[:, here]], axis=0)
        v_all = jnp.concatenate([before[:, there], values[:, here]], axis=0)
        for h in range(g * group, (g + 1) * group):
            cols = slice(h * HEAD_DIM, (h + 1) * HEAD_DIM)
            scores = lax.dot_general(
                q[:, cols], k_all, (((1,), (1,)), ((), ())), preferred_element_type=F32
            )
            scores = scores * HEAD_DIM**-0.5 - slopes[:, h : h + 1] * far
            scores = jnp.where(allowed, scores, -jnp.inf)
            sink = sinks[:, h : h + 1]
            peak = jnp.maximum(jnp.max(scores, axis=1, keepdims=True), sink)
            probs = jnp.exp(scores - peak)
            total = jnp.sum(probs, axis=1, keepdims=True) + jnp.exp(sink - peak)
            mixed = jnp.dot(probs.astype(BF), v_all, preferred_element_type=F32)
            attended[:, cols] = (mixed / total).astype(BF)
    for j in range(tps // 2):
        block = slice(j * quarter, (j + 1) * quarter)
        base = (y ^ j) * 2
        for ref, side in ((keep, core), (give, 1 - core)):
            at_col = pl.multiple_of((base + side) * quarter, quarter)
            ref[:, block] = jnp.dot(
                attended[...], weight[:, pl.ds(at_col, quarter)], preferred_element_type=F32
            ).astype(BF)


def expert_body(n_pieces, *refs):
    own, other = refs[:n_pieces], refs[n_pieces : 2 * n_pieces]
    gain, gate, up, down, keep, give, x, act = refs[2 * n_pieces :]
    _, y, _ = place()
    rows, width = keep.shape[1], keep.shape[2]
    depth = x.shape[1]
    for half, pieces in enumerate((own, other)):
        square = jnp.zeros((rows, 1), F32)
        for piece in pieces:
            for p in range(piece.shape[0]):
                part = piece[p].astype(F32)
                square = square + jnp.sum(part * part, axis=1, keepdims=True)
        scale = lax.rsqrt(square * (1.0 / depth) + 1e-06)
        j = 0
        for piece in pieces:
            for p in range(piece.shape[0]):
                cols = pl.ds(pl.multiple_of((y ^ j) * width, width), width)
                part = piece[p].astype(F32) * scale * gain[:, cols]
                x[half * rows : (half + 1) * rows, cols] = part.astype(BF)
                j += 1
    block = min(256, gate.shape[1])
    for lo in range(0, gate.shape[1], block):
        cols = slice(lo, lo + block)
        gate_pre = jnp.dot(x[...], gate[:, cols], preferred_element_type=F32)
        up_pre = jnp.dot(x[...], up[:, cols], preferred_element_type=F32)
        act[:, cols] = (gate_pre / (1.0 + jnp.exp(-gate_pre)) * up_pre).astype(BF)
    for j in range(keep.shape[0]):
        step = min(256, width)
        for lo in range(0, width, step):
            at_col = pl.multiple_of((y ^ j) * width + lo, step)
            part = jnp.dot(act[...], down[:, pl.ds(at_col, step)], preferred_element_type=F32)
            keep[j, :, lo : lo + step] = part[:rows].astype(BF)
            give[j, :, lo : lo + step] = part[rows:].astype(BF)


def assemble_body(*refs):
    own, other, out = refs[: len(refs) // 2], refs[len(refs) // 2 : -1], refs[-1]
    _, y, core = place()
    for pieces, side in ((own, core), (other, 1 - core)):
        j = 0
        for piece in pieces:
            width = piece.shape[2]
            for p in range(piece.shape[0]):
                at_col = pl.multiple_of(((y ^ j) * 2 + side) * width, width)
                out[:, pl.ds(at_col, width)] = piece[p]
                j += 1


def per_device(
    queries,
    key_rows,
    value_rows,
    sink_logits,
    out_weight,
    residual,
    norm_gain,
    routes,
    route_weights,
    gate_weight,
    up_weight,
    down_weight,
):
    sps, tps = lax.axis_size("sp"), lax.axis_size("tp")
    at, _, core = place()
    rows, width = residual.shape
    ys, quarter = tps // 2, width // tps
    half = sps // 2
    cap = 2 * rows * TOP // sps

    def swap_core(x):
        return lax.ppermute(x, "tp", [(i, i ^ 1) for i in range(tps)])

    def swap_y(x, bit):
        return lax.ppermute(x, "tp", [(i, i ^ (2 * bit)) for i in range(tps)])

    def swap_sp(x, k):
        pairs = []
        for i in range(sps):
            for j in range(tps):
                to = i ^ (2 * (half - 1 - k) + j % 2)
                pairs.append((i * tps + j, to * tps + j))
        return lax.ppermute(x, ("sp", "tp"), pairs)

    def spread_y(x):
        held, bit = [x[None]], 1
        while bit < ys:
            held.append(swap_y(jnp.concatenate(held) if len(held) > 1 else held[0], bit))
            bit *= 2
        return held

    def fold_y(x):
        bit = ys // 2
        while bit >= 1:
            x = x[:bit] + swap_y(x[bit:].astype(BF), bit).astype(F32)
            bit //= 2
        return x[0]

    rim = jnp.concatenate([key_rows, value_rows], axis=1)
    before = lax.ppermute(rim, "sp", [(i, i + 1) for i in range(sps - 1)])

    pick, comb = kernel_call(
        functools.partial(route_body, half, cap),
        (struct(half * cap, rows), struct(2, 2, half * cap, rows)),
    )(routes.T, route_weights.T)

    keep, give = kernel_call(
        functools.partial(attend_body, tps),
        (struct(rows, width // 2), struct(rows, width // 2)),
        [pltpu.VMEM((rows, queries.shape[1]), BF)],
    )(queries, key_rows, value_rows, before, sink_logits[None], out_weight)
    chip = keep.astype(F32) + swap_core(give).astype(F32)
    head_total = fold_y(jnp.stack(jnp.split(chip, ys, axis=1)))
    here = lax.dynamic_slice_in_dim(residual, lax.axis_index("tp") * quarter, quarter, 1)
    mixed = (here.astype(F32) + head_total).astype(BF)

    partner = swap_core(mixed)
    ordered = jnp.concatenate(
        [jnp.where(core == 0, mixed, partner), jnp.where(core == 0, partner, mixed)], axis=1
    )
    outgoing = jnp.dot(pick, ordered, preferred_element_type=F32).astype(BF)

    chunks = min(CHUNKS, half)
    per = half // chunks
    arrived = [
        [swap_sp(outgoing[k * cap : (k + 1) * cap], k) for k in range(c * per, (c + 1) * per)]
        for c in range(chunks)
    ]
    back = []
    for c in range(chunks):
        own = spread_y(jnp.concatenate(arrived[c]))
        other = [swap_core(piece) for piece in own]
        keep, give = kernel_call(
            functools.partial(expert_body, len(own)),
            (struct(ys, per * cap, 2 * quarter), struct(ys, per * cap, 2 * quarter)),
            [
                pltpu.VMEM((2 * per * cap, width), BF),
                pltpu.VMEM((2 * per * cap, gate_weight.shape[2]), BF),
            ],
        )(*own, *other, norm_gain[None], gate_weight[0], up_weight[0], down_weight[0])
        result = fold_y(keep.astype(F32) + swap_core(give).astype(F32)).astype(BF)
        for k in range(per):
            back.append(swap_sp(result[k * cap : (k + 1) * cap], c * per + k))
    returned = jnp.concatenate(back)
    low, high = returned[:, :quarter], returned[:, quarter:]
    mine = jnp.where(core == 0, low, high)
    others = swap_core(jnp.where(core == 0, high, low))
    total = mixed.astype(F32)
    for part, table in ((mine, 0), (others, 1)):
        for level in range(2):
            total = total + lax.dot_general(
                comb[table, level], part, (((0,), (0,)), ((), ())), preferred_element_type=F32
            )
    final = spread_y(total.astype(BF))
    final_other = [swap_core(piece) for piece in final]
    return kernel_call(assemble_body, struct(rows, width))(*final, *final_other)


def solution(mesh):
    placed = (
        P("sp", "tp"),
        P("sp", "tp"),
        P("sp", "tp"),
        P("tp"),
        P("tp", None),
        P("sp", None),
        P(),
        P("sp", None),
        P("sp", None),
        P("sp", None, "tp"),
        P("sp", None, "tp"),
        P("sp", "tp", None),
    )
    return jax.shard_map(
        per_device, mesh=mesh, in_specs=placed, out_specs=P("sp", None), check_vma=False
    )
```
